32 devices in a mesh: sp: 16 (over z, y, x), tp: 2 (over core).
Axes of the slice: x: 2, y: 2, z: 4, core: 2. Of those that a mesh axis runs over, the one named last changes fastest.
Arguments:
- stream: bfloat16 [2048, 2048], P('sp'), may hold values from -6 to 6
- query_narrow: bfloat16 [2048, 512], P('sp', 'tp'), may hold values from -7 to 7
- query_broad: bfloat16 [2048, 1024], P('sp', 'tp'), may hold values from -7 to 7
- key_narrow: bfloat16 [2048, 512], P('sp', 'tp'), may hold values from -7 to 7
- key_broad: bfloat16 [2048, 1024], P('sp', 'tp'), may hold values from -7 to 7
- value_narrow: bfloat16 [2048, 512], P('sp', 'tp'), may hold values from -6 to 6
- value_broad: bfloat16 [2048, 1024], P('sp', 'tp'), may hold values from -6 to 6
- key_offsets: float32 [2048, 16], P('sp', 'tp'), may hold values from -20 to 0
- out_narrow: bfloat16 [512, 2048], P('tp'), may hold values from -0.4375 to 0.4375
- out_broad: bfloat16 [1024, 2048], P('tp'), may hold values from -0.4375 to 0.4375
- norm_gain: float32 [2048], replicated, may hold values from 0.1 to 1.9
- gate_weight: bfloat16 [2048, 3072], P('sp', 'tp'), may hold values from -0.125 to 0.125
- up_weight: bfloat16 [2048, 3072], P('sp', 'tp'), may hold values from -0.125 to 0.125
- down_weight: bfloat16 [3072, 2048], P('tp', 'sp'), may hold values from -0.21875 to 0.21875
Outputs:
- result: bfloat16 [2048, 2048], P(('sp', 'tp'))
The draws below stay inside these ranges and needn't reach their ends.
All inputs are finite; a program needn't handle non-finite values.
Results may differ from the reference program's by a relative error of at most 0.028.
Values may be sent and summed in bfloat16 or wider, within the bound.
A program may use at most 64 MiB of HBM per device.

```python
import jax
import jax.numpy as jnp
from jax import lax

D = 2048
FF = 3072
NARROW_HEADS = 8
NARROW_SIZE = 64
BROAD_HEADS = 8
BROAD_SIZE = 128
TOK_DEV = 128
SEQUENCE_TOKENS = 2048
N_TP = 2


def draw_key_offsets(key, part):
    parallel_flows = jax.random.split(jax.random.fold_in(key, 17), 6)
    column_indices = 2 * NARROW_HEADS
    fast_share = 0.5
    spread = 0.7
    fast = jax.random.uniform(parallel_flows[0], (column_indices,), jnp.float32) < fast_share
    slow_base = -2.0 - jnp.log(jnp.float32(SEQUENCE_TOKENS)) + jax.random.uniform(parallel_flows[1], (column_indices,), jnp.float32, -0.5, 0.5)
    base = jnp.where(fast, -3.5, slow_base)
    shifts = jax.random.uniform(parallel_flows[2], (SEQUENCE_TOKENS // TOK_DEV, 1, column_indices), jnp.float32, -spread, spread)
    moved_forward = (base[None, None, :] + shifts + jnp.zeros((SEQUENCE_TOKENS // TOK_DEV, TOK_DEV, column_indices), jnp.float32)).reshape(SEQUENCE_TOKENS, column_indices)
    coarse_estimate = jax.random.uniform(parallel_flows[3], (SEQUENCE_TOKENS, column_indices), jnp.float32, -0.5, 0.5)
    arrival_group = jax.random.uniform(parallel_flows[4], (SEQUENCE_TOKENS, column_indices), jnp.float32) < 4.0 / SEQUENCE_TOKENS
    arrival_value = jax.random.uniform(parallel_flows[5], (SEQUENCE_TOKENS, column_indices), jnp.float32, -2.5, -1.0)
    return jnp.where(arrival_group, arrival_value, moved_forward + coarse_estimate).astype(jnp.float32)


def steps_of(own_key, dims, shards, low, high):
    factor_of, own = 1.0, jax.random.fold_in(own_key, 6)
    for position, blocks in shards:
        steps = jnp.exp(jax.random.uniform(jax.random.fold_in(own, position), (blocks,), jnp.float32, low / len(shards), high / len(shards)))
        factor_of = factor_of * jnp.repeat(steps, dims[position] // blocks).reshape([-1 if axis == position else 1 for axis in range(len(dims))])
    return factor_of


def noise(key, extent, width, limit, cuts=(), kind=jnp.bfloat16):
    array = jax.random.normal(key, extent, jnp.float32) * width
    if len(cuts) > 0:
        array = steps_of(key, extent, cuts, -0.22, 0.18) * array
    return jnp.clip(array, min=-limit, max=limit).astype(kind)


def setup_inputs(seed: int = 0) -> dict:
    seeds = jax.random.split(jax.random.key(seed), 15)
    return {
        "stream": noise(seeds[0], (SEQUENCE_TOKENS, D), 1.0, 6.0, ((0, 16),)),
        "query_narrow": noise(seeds[1], (SEQUENCE_TOKENS, NARROW_HEADS * NARROW_SIZE), 1.2, 7.0, ((0, 16), (1, 2))),
        "query_broad": noise(seeds[2], (SEQUENCE_TOKENS, BROAD_HEADS * BROAD_SIZE), 1.2, 7.0, ((0, 16), (1, 2))),
        "key_narrow": noise(seeds[3], (SEQUENCE_TOKENS, NARROW_HEADS * NARROW_SIZE), 1.2, 7.0, ((0, 16), (1, 2))),
        "key_broad": noise(seeds[4], (SEQUENCE_TOKENS, BROAD_HEADS * BROAD_SIZE), 1.2, 7.0, ((0, 16), (1, 2))),
        "value_narrow": noise(seeds[5], (SEQUENCE_TOKENS, NARROW_HEADS * NARROW_SIZE), 1.0, 6.0, ((0, 16), (1, 2))),
        "value_broad": noise(seeds[6], (SEQUENCE_TOKENS, BROAD_HEADS * BROAD_SIZE), 1.0, 6.0, ((0, 16), (1, 2))),
        "key_offsets": draw_key_offsets(jax.random.fold_in(seeds[14], 71), 0),
        "out_narrow": noise(seeds[8], (NARROW_HEADS * NARROW_SIZE, D), ((NARROW_HEADS * NARROW_SIZE + BROAD_HEADS * BROAD_SIZE) // 9) ** -0.5, 0.4375, ((0, 2),)),
        "out_broad": noise(seeds[9], (BROAD_HEADS * BROAD_SIZE, D), ((NARROW_HEADS * NARROW_SIZE + BROAD_HEADS * BROAD_SIZE) // 9) ** -0.5, 0.4375, ((0, 2),)),
        "norm_gain": jnp.clip(1.0 + 0.18 * jax.random.normal(seeds[10], (D,), jnp.float32), 0.1, 1.9),
        "gate_weight": noise(seeds[11], (D, FF), D ** -0.5, 0.125, ((0, 16), (1, 2))),
        "up_weight": noise(seeds[12], (D, FF), D ** -0.5, 0.125, ((0, 16), (1, 2))),
        "down_weight": noise(seeds[13], (FF, D), (FF // 4) ** -0.5, 0.21875, ((0, 2), (1, 16))),
    }


def stick_heads(query, keys, values, offsets, heads, size):
    total = query.shape[0]
    qblock = 512 if total % 512 == 0 else total
    scale = size ** (-0.5)
    pieces = []
    for head in range(heads):
        query_head = query[:, head * size:(head + 1) * size]
        key_head = keys[:, head * size:(head + 1) * size]
        value_head = values[:, head * size:(head + 1) * size]
        offset_head = offsets[:, head]

        def one_block(index):
            first = (index * qblock).astype(jnp.int32)
            rows_q = lax.dynamic_slice_in_dim(query_head, first, qblock, 0)
            logits = jnp.dot(rows_q, jnp.transpose(key_head), preferred_element_type=jnp.float32) * scale + offset_head[None, :]
            tpos = first + jnp.arange(qblock, dtype=jnp.int32)
            spos = jnp.arange(total, dtype=jnp.int32)
            causal = spos[None, :] < tpos[:, None]
            lognot = jnp.where(causal, jax.nn.log_sigmoid(-logits), 0.0)
            later = lax.cumsum(lognot, axis=1, reverse=True) - lognot
            weights = jnp.where(causal, jnp.exp(jax.nn.log_sigmoid(logits) + later), 0.0).astype(jnp.bfloat16)
            return jnp.dot(weights, value_head, preferred_element_type=jnp.float32)
        blocks = lax.map(one_block, jnp.arange(total // qblock, dtype=jnp.int32))
        pieces.append(blocks.reshape(total, size).astype(jnp.bfloat16))
    return jnp.concatenate(pieces, axis=1)

def rounded(value):
    return lax.optimization_barrier(value.astype(jnp.bfloat16)).astype(jnp.float32)

def reference(stream, query_narrow, query_broad, key_narrow, key_broad, value_narrow, value_broad, key_offsets, out_narrow, out_broad, norm_gain, gate_weight, up_weight, down_weight):
    attended_narrow = stick_heads(query_narrow, key_narrow, value_narrow, key_offsets[:, 0::2], NARROW_HEADS, NARROW_SIZE)
    attended_broad = stick_heads(query_broad, key_broad, value_broad, key_offsets[:, 1::2], BROAD_HEADS, BROAD_SIZE)
    width_narrow = NARROW_HEADS // N_TP * NARROW_SIZE
    width_broad = BROAD_HEADS // N_TP * BROAD_SIZE
    total = jnp.zeros((stream.shape[0], D), jnp.float32)
    for index in range(N_TP):
        part = jnp.dot(attended_narrow[:, index * width_narrow:(index + 1) * width_narrow], out_narrow[index * width_narrow:(index + 1) * width_narrow], preferred_element_type=jnp.float32)
        part = part + jnp.dot(attended_broad[:, index * width_broad:(index + 1) * width_broad], out_broad[index * width_broad:(index + 1) * width_broad], preferred_element_type=jnp.float32)
        total = total + rounded(part)
    mid = (stream.astype(jnp.float32) + total).astype(jnp.bfloat16)
    middle = mid.astype(jnp.float32)
    normed = (middle * lax.rsqrt(lax.optimization_barrier(jnp.mean(middle * middle, axis=1, keepdims=True)) + 1e-06) * norm_gain).astype(jnp.bfloat16)
    gate = jnp.dot(normed, gate_weight, preferred_element_type=jnp.float32)
    up = jnp.dot(normed, up_weight, preferred_element_type=jnp.float32)
    hidden = (jax.nn.silu(gate) * up).astype(jnp.bfloat16)
    hidden_width = FF // N_TP
    mixed = jnp.zeros((stream.shape[0], D), jnp.float32)
    for index in range(N_TP):
        part = jnp.dot(hidden[:, index * hidden_width:(index + 1) * hidden_width], down_weight[index * hidden_width:(index + 1) * hidden_width], preferred_element_type=jnp.float32)
        mixed = mixed + rounded(part)
    return (middle + mixed).astype(jnp.bfloat16)
```

```python
import functools

import jax
import jax.numpy as jnp
from jax import lax
from jax.experimental import pallas as pl
from jax.experimental.pallas import tpu as pltpu
from jax.sharding import PartitionSpec as P

NARROW_SIZE = 64
BROAD_SIZE = 128
WIDE = 128
norm_eps = 1e-06
MESH = pl.DeviceIdType.MESH


def greet(axis_peers):
    barrier = pltpu.get_barrier_semaphore()
    count = 0
    for peers, total in axis_peers:
        def signal(t, carry, peers=peers):
            pl.semaphore_signal(barrier, inc=1, device_id=peers(t), device_id_type=MESH)
            return carry

        lax.fori_loop(1, total, signal, 0)
        count += total - 1
    pl.semaphore_wait(barrier, count)


def attend_kernel(n, hp, rows, group, q_ref, kv_ref, off_ref, *rest):
    H = 2 * hp
    R = n // H
    weights_too = group > 0
    if weights_too:
        (gate_ref, up_ref, down_ref, att_ref, gate_all, up_all, down_all) = rest[:7]
        rest = rest[7:]
    else:
        att_ref = rest[0]
        rest = rest[1:]
    (kvbuf, offbuf, qbuf, obuf, tri, kv_s, kv_r, off_s, off_r, q_s, q_r, att_s, att_r) = rest[:13]
    me = lax.axis_index("sp")
    head = me // R
    sub = me % R

    def snake(b):
        v = b % (2 * R)
        return jnp.where(v < R, v, 2 * R - 1 - v)

    def block_of(i, r):
        return i * R + jnp.where(i % 2 == 0, r, R - 1 - r)

    def peer(t):
        return lax.rem(me + t, n)

    def kv_copy(d, slot_src, sem):
        return pltpu.make_async_remote_copy(
            src_ref=kv_ref.at[d // R], dst_ref=kvbuf.at[slot_src], send_sem=kv_s.at[sem],
            recv_sem=kv_r.at[slot_src], device_id={"sp": d}, device_id_type=MESH)

    def off_copy(d, slot_src, sem):
        return pltpu.make_async_remote_copy(
            src_ref=off_ref.at[d // R], dst_ref=offbuf.at[slot_src], send_sem=off_s.at[sem],
            recv_sem=off_r.at[slot_src], device_id={"sp": d}, device_id_type=MESH)

    def q_copy(h, d, slot):
        return pltpu.make_async_remote_copy(
            src_ref=q_ref.at[h], dst_ref=qbuf.at[slot], send_sem=q_s.at[h],
            recv_sem=q_r.at[slot], device_id={"sp": d}, device_id_type=MESH)

    def att_copy(i, d, h):
        return pltpu.make_async_remote_copy(
            src_ref=obuf.at[i], dst_ref=att_ref.at[h], send_sem=att_s.at[i],
            recv_sem=att_r.at[h], device_id={"sp": d}, device_id_type=MESH)

    if weights_too:
        (g_s, g_r, u_s, u_r, d_s, d_r) = rest[13:19]
        drows = gate_ref.shape[0]
        fcols = gate_all.shape[1]
        dcols = down_ref.shape[1]

        def w_pieces(d, src):
            part = pl.multiple_of((d % group) * fcols, 128)
            at_rows = pl.ds(pl.multiple_of(src * drows, 128), drows)
            at_cols = pl.ds(pl.multiple_of(src * dcols, 128), dcols)
            return (
                (gate_ref.at[:, pl.ds(part, fcols)], gate_all.at[at_rows, :], g_s, g_r),
                (up_ref.at[:, pl.ds(part, fcols)], up_all.at[at_rows, :], u_s, u_r),
                (down_ref.at[pl.ds(part, fcols), :], down_all.at[:, at_cols], d_s, d_r),
            )

        def w_copies(d, src, sem):
            return [
                pltpu.make_async_remote_copy(
                    src_ref=a, dst_ref=b, send_sem=ss.at[sem], recv_sem=rs.at[src],
                    device_id={"sp": d}, device_id_type=MESH)
                for a, b, ss, rs in w_pieces(d, src)
            ]

        def w_local():
            return [pltpu.make_async_copy(a, b, rs.at[me]) for a, b, ss, rs in w_pieces(me, me)]

    greet([(lambda t: {"sp": peer(t)}, n)])

    def send_q(h, carry):
        d = h * R + snake(me)

        @pl.when(d != me)
        def _():
            q_copy(h, d, me // R).start()

        @pl.when(d == me)
        def _():
            pltpu.make_async_copy(q_ref.at[h], qbuf.at[me // R], q_r.at[me // R]).start()

        return carry

    def send_kv(t, carry):
        d = peer(t)
        kv_copy(d, me, t).start()
        off_copy(d, me, t).start()
        return carry

    lax.fori_loop(1, n, send_kv, 0)
    lax.fori_loop(0, H, send_q, 0)
    pltpu.make_async_copy(kv_ref.at[head], kvbuf.at[me], kv_r.at[me]).start()
    pltpu.make_async_copy(off_ref.at[head], offbuf.at[me], off_r.at[me]).start()
    if weights_too:
        def send_w(t, carry):
            for c in w_copies(peer(t), me, t):
                c.start()
            return carry

        lax.fori_loop(1, n, send_w, 0)
        for c in w_local():
            c.start()

    row = lax.broadcasted_iota(jnp.int32, (WIDE, WIDE), 0)
    col = lax.broadcasted_iota(jnp.int32, (WIDE, WIDE), 1)
    strict = jnp.where(row > col, 1.0, 0.0).astype(jnp.bfloat16)
    ones = jnp.ones((WIDE, WIDE), jnp.bfloat16)
    half = jnp.concatenate([strict, ones], axis=1)
    tri[...] = jnp.concatenate([half, half], axis=0)

    def wait_kv(t, carry):
        src = peer(t)
        kv_copy(src, src, t).wait_recv()
        off_copy(src, src, t).wait_recv()
        return carry

    lax.fori_loop(1, n, wait_kv, 0)
    pltpu.make_async_copy(kv_ref.at[head], kvbuf.at[me], kv_r.at[me]).wait()
    pltpu.make_async_copy(off_ref.at[head], offbuf.at[me], off_r.at[me]).wait()

    scale = jnp.where(head < hp, jnp.float32(NARROW_SIZE ** (-0.5)), jnp.float32(BROAD_SIZE ** (-0.5)))
    wide = 4 if n % 4 == 0 else 1

    def one_query(i, carry):
        b = block_of(i, sub)

        @pl.when(b != me)
        def _():
            q_copy(head, b, i).wait_recv()

        @pl.when(b == me)
        def _():
            pltpu.make_async_copy(q_ref.at[head], qbuf.at[i], q_r.at[i]).wait()

        q = qbuf[i]
        chunks = b // wide + 1

        def one_chunk(step, state):
            acc, later = state
            c = chunks - 1 - step
            held = kvbuf[pl.ds(c * wide, wide)]
            pieces = [None] * wide
            for k in reversed(range(wide)):
                logits = lax.dot_general(
                    q, held[k, 0], (((1,), (1,)), ((), ())), preferred_element_type=jnp.float32
                ) * scale + offbuf[c * wide + k][0:1, :]
                causal = (c * wide + k) * rows + col < b * rows + row
                soft = jnp.maximum(logits, 0.0) + jnp.log(1.0 + jnp.exp(-jnp.abs(logits)))
                masked = jnp.where(causal, soft, 0.0)
                high = masked.astype(jnp.bfloat16)
                low = (masked - high.astype(jnp.float32)).astype(jnp.bfloat16)
                sums = jnp.dot(
                    jnp.concatenate([high, low], axis=1), tri[...], preferred_element_type=jnp.float32
                )
                exponent = (logits - soft) - (sums[:, :WIDE] + later)
                pieces[k] = jnp.where(causal, jnp.exp(exponent), 0.0).astype(jnp.bfloat16)
                later = later + sums[:, WIDE:]
            weights = jnp.concatenate(pieces, axis=1)
            values = held[:, 1].reshape(wide * rows, WIDE)
            acc = acc + jnp.dot(weights, values, preferred_element_type=jnp.float32)
            return acc, later

        zero = jnp.zeros((rows, WIDE), jnp.float32)
        acc, _ = lax.fori_loop(0, chunks, one_chunk, (zero, zero))
        obuf[i] = acc.astype(jnp.bfloat16)

        @pl.when(b != me)
        def _():
            att_copy(i, b, head).start()

        @pl.when(b == me)
        def _():
            pltpu.make_async_copy(obuf.at[i], att_ref.at[head], att_r.at[head]).start()

        return carry

    lax.fori_loop(0, H, one_query, 0)

    def wait_sends(t, carry):
        d = peer(t)
        kv_copy(d, me, t).wait_send()
        off_copy(d, me, t).wait_send()
        if weights_too:
            for c in w_copies(d, me, t):
                c.wait_send()
            for c in w_copies(d, d, t):
                c.wait_recv()
        return carry

    lax.fori_loop(1, n, wait_sends, 0)
    if weights_too:
        for c in w_local():
            c.wait()

    def wait_att(h, carry):
        d = h * R + snake(me)
        b = block_of(h, sub)

        @pl.when(d != me)
        def _():
            q_copy(h, d, me // R).wait_send()
            att_copy(0, d, h).wait_recv()

        @pl.when(d == me)
        def _():
            pltpu.make_async_copy(obuf.at[0], att_ref.at[h], att_r.at[h]).wait()

        @pl.when(b != me)
        def _():
            att_copy(h, b, head).wait_send()

        return carry

    lax.fori_loop(0, H, wait_att, 0)


def attend(n, hp, rows, group, q, kv, off, weights):
    H = 2 * hp
    dma = pltpu.SemaphoreType.DMA
    vmem = pl.BlockSpec(memory_space=pltpu.VMEM)
    hbm = pl.BlockSpec(memory_space=pl.ANY)
    out_shape = [jax.ShapeDtypeStruct((H, rows, WIDE), jnp.bfloat16)]
    scratch = [
        pltpu.VMEM((n, 2, rows, WIDE), jnp.bfloat16),
        pltpu.VMEM((n, 8, WIDE), jnp.float32),
        pltpu.VMEM((H, rows, WIDE), jnp.bfloat16),
        pltpu.VMEM((H, rows, WIDE), jnp.bfloat16),
        pltpu.VMEM((2 * WIDE, 2 * WIDE), jnp.bfloat16),
        dma((n,)), dma((n,)), dma((n,)), dma((n,)), dma((H,)), dma((H,)), dma((H,)), dma((H,)),
    ]
    args = [q, kv, off]
    specs = [vmem] * 3
    if group:
        gate, up, down = weights
        cols = gate.shape[1] // group
        out_shape += [jax.ShapeDtypeStruct((gate.shape[0] * n, cols), jnp.bfloat16)] * 2
        out_shape += [jax.ShapeDtypeStruct((cols, down.shape[1] * n), jnp.bfloat16)]
        scratch += [dma((n,))] * 6
        args += [gate, up, down]
        specs += [hbm] * 3
    return pl.pallas_call(
        functools.partial(attend_kernel, n, hp, rows, group),
        out_shape=out_shape,
        in_specs=specs,
        out_specs=[hbm] * len(out_shape),
        scratch_shapes=scratch,
        compiler_params=pltpu.CompilerParams(
            collective_id=0, has_side_effects=True, vmem_limit_bytes=40 * 1024 * 1024
        ),
    )(*args)


def mix_kernel(a, T, hp, att_ref, on_ref, ob_ref, stream_ref, gain_ref, gate_ref, up_ref, down_ref,
               out_ref, pbuf, prec, mid, xs, pb, ps, p_s, p_r, x_s, x_r, r_s, r_r):
    G = a * T
    me = lax.axis_index("sp")
    j = lax.axis_index("tp")
    base = (me // a) * a
    g = (me - base) * T + j
    share = out_ref.shape[0]

    def place(e):
        return {"sp": base + e // T, "tp": e % T}

    def other(t):
        return lax.rem(g + t, G)

    greet([(lambda t: place(other(t)), G)])

    cut = [att_ref[h][:, :NARROW_SIZE] for h in range(hp)]
    part = jnp.dot(jnp.concatenate(cut, axis=1), on_ref[...], preferred_element_type=jnp.float32)
    part = part + jnp.dot(
        jnp.concatenate([att_ref[hp + h] for h in range(hp)], axis=1), ob_ref[...],
        preferred_element_type=jnp.float32,
    )
    pbuf[...] = part.astype(jnp.bfloat16).reshape(pbuf.shape)

    def p_copy(to, src, t):
        return pltpu.make_async_remote_copy(
            src_ref=pbuf.at[to], dst_ref=prec.at[src], send_sem=p_s.at[t], recv_sem=p_r.at[src],
            device_id={"tp": to}, device_id_type=MESH)

    for t in range(1, T):
        p_copy(lax.rem(j + t, T), j, t).start()
    total = pbuf[j].astype(jnp.float32)
    for t in range(1, T):
        src = lax.rem(j + t, T)
        p_copy(src, src, t).wait_recv()
        total = total + prec[src].astype(jnp.float32)
    own = pl.ds(pl.multiple_of(j * share, share), share)
    mid[...] = (stream_ref[own, :].astype(jnp.float32) + total).astype(jnp.bfloat16)
    middle = mid[...].astype(jnp.float32)
    scaled = middle * lax.rsqrt(jnp.mean(middle * middle, axis=1, keepdims=True) + norm_eps)
    xs[g] = (scaled * gain_ref[...]).astype(jnp.bfloat16)

    def x_copy(e, src, t):
        return pltpu.make_async_remote_copy(
            src_ref=xs.at[src], dst_ref=xs.at[src], send_sem=x_s.at[t], recv_sem=x_r.at[src],
            device_id=place(e), device_id_type=MESH)

    def r_copy(e, src):
        return pltpu.make_async_remote_copy(
            src_ref=pb.at[e], dst_ref=ps.at[src], send_sem=r_s.at[e], recv_sem=r_r.at[src],
            device_id=place(e), device_id_type=MESH)

    def send_x(t, carry):
        x_copy(other(t), g, t).start()
        return carry

    lax.fori_loop(1, G, send_x, 0)

    def one_member(k, carry):
        m = lax.rem(me - base + k, a)
        for s in range(T):
            e = m * T + s

            @pl.when(e != g)
            def _():
                x_copy(e, e, 0).wait_recv()

        x = xs[pl.ds(m * T, T)].reshape(T * share, xs.shape[2])
        gate = jnp.dot(x, gate_ref[...], preferred_element_type=jnp.float32)
        up = jnp.dot(x, up_ref[...], preferred_element_type=jnp.float32)
        hidden = (gate / (1.0 + jnp.exp(-gate)) * up).astype(jnp.bfloat16)
        mixed = jnp.dot(hidden, down_ref[...], preferred_element_type=jnp.float32)
        pb[pl.ds(m * T, T)] = mixed.astype(jnp.bfloat16).reshape(T, share, mixed.shape[1])
        for s in range(T):
            e = m * T + s

            @pl.when(e != g)
            def _():
                r_copy(e, g).start()

        return carry

    lax.fori_loop(0, a, one_member, 0)
    total = pb[g].astype(jnp.float32)
    for t in range(1, G):
        e = other(t)
        r_copy(e, e).wait_recv()
        total = total + ps[e].astype(jnp.float32)
    out_ref[...] = (mid[...].astype(jnp.float32) + total).astype(jnp.bfloat16)
    for t in range(1, T):
        p_copy(lax.rem(j + t, T), j, t).wait_send()

    def finish(t, carry):
        x_copy(other(t), g, t).wait_send()
        r_copy(other(t), g).wait_send()
        return carry

    lax.fori_loop(1, G, finish, 0)


def mix(a, T, hp, att, out_narrow, out_broad, stream, gain, gate, up, down):
    G = a * T
    rows, width = stream.shape
    share = rows // T
    dma = pltpu.SemaphoreType.DMA
    block = pltpu.VMEM((G, share, width), jnp.bfloat16)
    pair = pltpu.VMEM((T, share, width), jnp.bfloat16)
    return pl.pallas_call(
        functools.partial(mix_kernel, a, T, hp),
        out_shape=jax.ShapeDtypeStruct((share, width), jnp.bfloat16),
        in_specs=[pl.BlockSpec(memory_space=pltpu.VMEM)] * 8,
        out_specs=pl.BlockSpec(memory_space=pltpu.VMEM),
        scratch_shapes=[
            pair, pair, pltpu.VMEM((share, width), jnp.bfloat16), block, block, block,
            dma((T,)), dma((T,)), dma((G,)), dma((G,)), dma((G,)), dma((G,)),
        ],
        compiler_params=pltpu.CompilerParams(
            collective_id=1, has_side_effects=True, vmem_limit_bytes=60 * 1024 * 1024
        ),
    )(att, out_narrow, out_broad, stream, gain.reshape(1, width), gate, up, down)


def split_heads(array, heads, size):
    cut = jnp.transpose(array.reshape(array.shape[0], heads, size), (1, 0, 2))
    return jnp.pad(cut, ((0, 0), (0, 0), (0, WIDE - size)))


def local(n, T,
    stream,
    query_narrow,
    query_broad,
    key_narrow,
    key_broad,
    value_narrow,
    value_broad,
    key_offsets,
    out_narrow,
    out_broad,
    norm_gain,
    gate_weight,
    up_weight,
    down_weight,
):
    rows = stream.shape[0]
    hp = query_narrow.shape[1] // NARROW_SIZE

    def both(narrow, broad):
        return jnp.concatenate(
            [split_heads(narrow, hp, NARROW_SIZE), split_heads(broad, hp, BROAD_SIZE)], axis=0
        )

    q = both(query_narrow, query_broad)
    kv = jnp.stack([both(key_narrow, key_broad), both(value_narrow, value_broad)], axis=1)
    off = jnp.transpose(jnp.concatenate([key_offsets[:, 0::2], key_offsets[:, 1::2]], axis=1))
    off = jnp.broadcast_to(off[:, None, :], (2 * hp, 8, rows))
    group = 0
    if gate_weight.shape[0] % 128 == 0 and down_weight.shape[1] % 128 == 0:
        for a in (1, 2, 4):
            if n % a == 0 and gate_weight.shape[1] % (128 * a) == 0:
                group = a
    if group:
        att, gate_all, up_all, down_all = attend(
            n, hp, rows, group, q, kv, off, (gate_weight, up_weight, down_weight)
        )
        return mix(
            group, T, hp, att, out_narrow, out_broad, stream, norm_gain, gate_all, up_all, down_all
        )
    att = attend(n, hp, rows, 0, q, kv, off, None)[0]
    attended_narrow = jnp.transpose(att[:hp, :, :NARROW_SIZE], (1, 0, 2)).reshape(rows, -1)
    attended_broad = jnp.transpose(att[hp:], (1, 0, 2)).reshape(rows, -1)
    share = rows // T
    own = lax.axis_index("tp") * share
    summed = lax.psum_scatter(
        (
            jnp.dot(attended_narrow, out_narrow, preferred_element_type=jnp.float32)
            + jnp.dot(attended_broad, out_broad, preferred_element_type=jnp.float32)
        ).astype(jnp.bfloat16),
        "tp",
        scatter_dimension=0,
        tiled=True,
    ).astype(jnp.float32)
    mid_own = (lax.dynamic_slice_in_dim(stream, own, share, 0).astype(jnp.float32) + summed).astype(
        jnp.bfloat16
    )
    middle = mid_own.astype(jnp.float32)
    scaled = middle * lax.rsqrt(jnp.mean(middle * middle, axis=1, keepdims=True) + norm_eps)
    normed = lax.all_gather((scaled * norm_gain).astype(jnp.bfloat16), "tp", axis=0, tiled=True)
    part_gate = lax.all_gather(gate_weight, "sp", axis=0, tiled=True)
    part_up = lax.all_gather(up_weight, "sp", axis=0, tiled=True)
    gate = jnp.dot(normed, part_gate, preferred_element_type=jnp.float32)
    up = jnp.dot(normed, part_up, preferred_element_type=jnp.float32)
    hidden = (jax.nn.silu(gate) * up).astype(jnp.bfloat16)
    down_full = lax.all_gather(down_weight, "sp", axis=1, tiled=True)
    mixed = lax.psum_scatter(
        jnp.dot(
            hidden,
            down_full,
            preferred_element_type=jnp.float32,
        ).astype(jnp.bfloat16),
        "tp",
        scatter_dimension=0,
        tiled=True,
    ).astype(jnp.float32)
    return (mid_own.astype(jnp.float32) + mixed).astype(jnp.bfloat16)


def solution(mesh):
    placed = (
        P("sp", None),
        P("sp", "tp"),
        P("sp", "tp"),
        P("sp", "tp"),
        P("sp", "tp"),
        P("sp", "tp"),
        P("sp", "tp"),
        P("sp", "tp"),
        P("tp", None),
        P("tp", None),
        P(),
        P("sp", "tp"),
        P("sp", "tp"),
        P("tp", "sp"),
    )
    body = functools.partial(local, mesh.shape["sp"], mesh.shape["tp"])
    return jax.shard_map(
        body, mesh=mesh, in_specs=placed, out_specs=P(("sp", "tp"), None), check_vma=False
    )
```

```python
import functools

import jax
import jax.numpy as jnp
from jax import lax
from jax.experimental import pallas as pl
from jax.experimental.pallas import tpu as pltpu
from jax.sharding import PartitionSpec as P

NARROW_SIZE = 64
BROAD_SIZE = 128
WIDE = 128
norm_eps = 1e-06
MESH = pl.DeviceIdType.MESH


def greet(axis_peers):
    barrier = pltpu.get_barrier_semaphore()
    count = 0
    for peers, total in axis_peers:
        def signal(t, carry, peers=peers):
            pl.semaphore_signal(barrier, inc=1, device_id=peers(t), device_id_type=MESH)
            return carry

        lax.fori_loop(1, total, signal, 0)
        count += total - 1
    pl.semaphore_wait(barrier, count)


def attend_kernel(n, hp, rows, group, q_ref, kv_ref, off_ref, *rest):
    H = 2 * hp
    R = n // H
    weights_too = group > 0
    if weights_too:
        (gate_ref, up_ref, down_ref, att_ref, gate_all, up_all, down_all) = rest[:7]
        rest = rest[7:]
    else:
        att_ref = rest[0]
        rest = rest[1:]
    (kvbuf, offbuf, qbuf, obuf, tri, kv_s, kv_r, off_s, off_r, q_s, q_r, att_s, att_r) = rest[:13]
    me = lax.axis_index("sp")
    head = me // R
    sub = me % R

    def snake(b):
        v = b % (2 * R)
        return jnp.where(v < R, v, 2 * R - 1 - v)

    def block_of(i, r):
        return i * R + jnp.where(i % 2 == 0, r, R - 1 - r)

    def peer(t):
        return lax.rem(me + t, n)

    def kv_copy(d, slot_src, sem):
        return pltpu.make_async_remote_copy(
            src_ref=kv_ref.at[d // R], dst_ref=kvbuf.at[slot_src], send_sem=kv_s.at[sem],
            recv_sem=kv_r.at[slot_src], device_id={"sp": d}, device_id_type=MESH)

    def off_copy(d, slot_src, sem):
        return pltpu.make_async_remote_copy(
            src_ref=off_ref.at[d // R], dst_ref=offbuf.at[slot_src], send_sem=off_s.at[sem],
            recv_sem=off_r.at[slot_src], device_id={"sp": d}, device_id_type=MESH)

    def q_copy(h, d, slot):
        return pltpu.make_async_remote_copy(
            src_ref=q_ref.at[h], dst_ref=qbuf.at[slot], send_sem=q_s.at[h],
            recv_sem=q_r.at[slot], device_id={"sp": d}, device_id_type=MESH)

    def att_copy(i, d, h):
        return pltpu.make_async_remote_copy(
            src_ref=obuf.at[i], dst_ref=att_ref.at[h], send_sem=att_s.at[i],
            recv_sem=att_r.at[h], device_id={"sp": d}, device_id_type=MESH)

    if weights_too:
        (g_s, g_r, u_s, u_r, d_s, d_r) = rest[13:19]
        drows = gate_ref.shape[0]
        fcols = gate_all.shape[1]
        dcols = down_ref.shape[1]

        cols = n // group
        mine, lane = me // cols, me % cols

        def at_rows(src):
            return pl.ds(pl.multiple_of(src * drows, 128), drows)

        def at_cols(src):
            return pl.ds(pl.multiple_of(src * dcols, 128), dcols)

        def landing(src):
            return (gate_all.at[at_rows(src), :], up_all.at[at_rows(src), :], down_all.at[:, at_cols(src)])

        def raw(member):
            part = pl.ds(pl.multiple_of(member * fcols, 128), fcols)
            return (gate_ref.at[:, part], up_ref.at[:, part], down_ref.at[part, :])

        def w_copies(sources, src, d, sem):
            return [
                pltpu.make_async_remote_copy(
                    src_ref=a, dst_ref=b, send_sem=ss.at[sem], recv_sem=rs.at[src],
                    device_id={"sp": d}, device_id_type=MESH)
                for a, b, ss, rs in zip(sources, landing(src), (g_s, u_s, d_s), (g_r, u_r, d_r))
            ]

        def w_local():
            return [
                pltpu.make_async_copy(a, b, rs.at[me])
                for a, b, rs in zip(raw(mine), landing(me), (g_r, u_r, d_r))
            ]

        def along(k):
            return lax.rem(mine + k, group)

        def beside(t):
            return lax.rem(lane + t, cols)

        def first_copies(k):
            return w_copies(raw(along(k)), me, along(k) * cols + lane, k)

        def own_copies(t):
            return w_copies(raw(mine), me, mine * cols + beside(t), group + t)

        def next_copies(k, t):
            src = along(k) * cols + lane
            return w_copies(landing(src), src, mine * cols + beside(t), group + k * cols + t)

    greet([(lambda t: {"sp": peer(t)}, n)])

    def send_q(h, carry):
        d = h * R + snake(me)

        @pl.when(d != me)
        def _():
            q_copy(h, d, me // R).start()

        @pl.when(d == me)
        def _():
            pltpu.make_async_copy(q_ref.at[h], qbuf.at[me // R], q_r.at[me // R]).start()

        return carry

    def send_kv(t, carry):
        d = peer(t)
        kv_copy(d, me, t).start()
        off_copy(d, me, t).start()
        return carry

    if weights_too:
        for k in range(1, group):
            for c in first_copies(k):
                c.start()
        for t in range(1, cols):
            for c in own_copies(t):
                c.start()
    lax.fori_loop(1, n, send_kv, 0)
    lax.fori_loop(0, H, send_q, 0)
    pltpu.make_async_copy(kv_ref.at[head], kvbuf.at[me], kv_r.at[me]).start()
    pltpu.make_async_copy(off_ref.at[head], offbuf.at[me], off_r.at[me]).start()
    if weights_too:
        for c in w_local():
            c.start()
        for k in range(1, group):
            src = along(k) * cols + lane
            for index, c in enumerate(w_copies(landing(src), src, src, k)):
                c.wait_recv()
                for t in range(1, cols):
                    next_copies(k, t)[index].start()

    row = lax.broadcasted_iota(jnp.int32, (WIDE, WIDE), 0)
    col = lax.broadcasted_iota(jnp.int32, (WIDE, WIDE), 1)
    strict = jnp.where(row > col, 1.0, 0.0).astype(jnp.bfloat16)
    ones = jnp.ones((WIDE, WIDE), jnp.bfloat16)
    half = jnp.concatenate([strict, ones], axis=1)
    tri[...] = jnp.concatenate([half, half], axis=0)

    def wait_kv(t, carry):
        src = peer(t)
        kv_copy(src, src, t).wait_recv()
        off_copy(src, src, t).wait_recv()
        return carry

    lax.fori_loop(1, n, wait_kv, 0)
    pltpu.make_async_copy(kv_ref.at[head], kvbuf.at[me], kv_r.at[me]).wait()
    pltpu.make_async_copy(off_ref.at[head], offbuf.at[me], off_r.at[me]).wait()

    scale = jnp.where(head < hp, jnp.float32(NARROW_SIZE ** (-0.5)), jnp.float32(BROAD_SIZE ** (-0.5)))
    wide = 4 if n % 4 == 0 else 1

    def one_query(i, carry):
        b = block_of(i, sub)

        @pl.when(b != me)
        def _():
            q_copy(head, b, i).wait_recv()

        @pl.when(b == me)
        def _():
            pltpu.make_async_copy(q_ref.at[head], qbuf.at[i], q_r.at[i]).wait()

        q = qbuf[i]
        chunks = b // wide + 1

        def one_chunk(step, state):
            acc, later = state
            c = chunks - 1 - step
            held = kvbuf[pl.ds(c * wide, wide)]
            pieces = [None] * wide
            for k in reversed(range(wide)):
                logits = lax.dot_general(
                    q, held[k, 0], (((1,), (1,)), ((), ())), preferred_element_type=jnp.float32
                ) * scale + offbuf[c * wide + k][0:1, :]
                causal = (c * wide + k) * rows + col < b * rows + row
                soft = jnp.maximum(logits, 0.0) + jnp.log(1.0 + jnp.exp(-jnp.abs(logits)))
                masked = jnp.where(causal, soft, 0.0)
                high = masked.astype(jnp.bfloat16)
                low = (masked - high.astype(jnp.float32)).astype(jnp.bfloat16)
                sums = jnp.dot(
                    jnp.concatenate([high, low], axis=1), tri[...], preferred_element_type=jnp.float32
                )
                exponent = (logits - soft) - (sums[:, :WIDE] + later)
                pieces[k] = jnp.where(causal, jnp.exp(exponent), 0.0).astype(jnp.bfloat16)
                later = later + sums[:, WIDE:]
            weights = jnp.concatenate(pieces, axis=1)
            values = held[:, 1].reshape(wide * rows, WIDE)
            acc = acc + jnp.dot(weights, values, preferred_element_type=jnp.float32)
            return acc, later

        zero = jnp.zeros((rows, WIDE), jnp.float32)
        acc, _ = lax.fori_loop(0, chunks, one_chunk, (zero, zero))
        obuf[i] = acc.astype(jnp.bfloat16)

        @pl.when(b != me)
        def _():
            att_copy(i, b, head).start()

        @pl.when(b == me)
        def _():
            pltpu.make_async_copy(obuf.at[i], att_ref.at[head], att_r.at[head]).start()

        return carry

    lax.fori_loop(0, H, one_query, 0)

    def wait_sends(t, carry):
        d = peer(t)
        kv_copy(d, me, t).wait_send()
        off_copy(d, me, t).wait_send()
        return carry

    lax.fori_loop(1, n, wait_sends, 0)
    if weights_too:
        for k in range(1, group):
            for c in first_copies(k):
                c.wait_send()
        for t in range(1, cols):
            for c in own_copies(t):
                c.wait_send()
            for k in range(group):
                src = along(k) * cols + beside(t)
                for c in w_copies(landing(src), src, src, 0):
                    c.wait_recv()
                if k:
                    for c in next_copies(k, t):
                        c.wait_send()
        for c in w_local():
            c.wait()

    def wait_att(h, carry):
        d = h * R + snake(me)
        b = block_of(h, sub)

        @pl.when(d != me)
        def _():
            q_copy(h, d, me // R).wait_send()
            att_copy(0, d, h).wait_recv()

        @pl.when(d == me)
        def _():
            pltpu.make_async_copy(obuf.at[0], att_ref.at[h], att_r.at[h]).wait()

        @pl.when(b != me)
        def _():
            att_copy(h, b, head).wait_send()

        return carry

    lax.fori_loop(0, H, wait_att, 0)


def attend(n, hp, rows, group, q, kv, off, weights):
    H = 2 * hp
    dma = pltpu.SemaphoreType.DMA
    vmem = pl.BlockSpec(memory_space=pltpu.VMEM)
    hbm = pl.BlockSpec(memory_space=pl.ANY)
    out_shape = [jax.ShapeDtypeStruct((H, rows, WIDE), jnp.bfloat16)]
    scratch = [
        pltpu.VMEM((n, 2, rows, WIDE), jnp.bfloat16),
        pltpu.VMEM((n, 8, WIDE), jnp.float32),
        pltpu.VMEM((H, rows, WIDE), jnp.bfloat16),
        pltpu.VMEM((H, rows, WIDE), jnp.bfloat16),
        pltpu.VMEM((2 * WIDE, 2 * WIDE), jnp.bfloat16),
        dma((n,)), dma((n,)), dma((n,)), dma((n,)), dma((H,)), dma((H,)), dma((H,)), dma((H,)),
    ]
    args = [q, kv, off]
    specs = [vmem] * 3
    if group:
        gate, up, down = weights
        cols = gate.shape[1] // group
        out_shape += [jax.ShapeDtypeStruct((gate.shape[0] * n, cols), jnp.bfloat16)] * 2
        out_shape += [jax.ShapeDtypeStruct((cols, down.shape[1] * n), jnp.bfloat16)]
        scratch += [dma((group + n,)), dma((n,))] * 3
        args += [gate, up, down]
        specs += [hbm] * 3
    return pl.pallas_call(
        functools.partial(attend_kernel, n, hp, rows, group),
        out_shape=out_shape,
        in_specs=specs,
        out_specs=[hbm] * len(out_shape),
        scratch_shapes=scratch,
        compiler_params=pltpu.CompilerParams(
            collective_id=0, has_side_effects=True, vmem_limit_bytes=40 * 1024 * 1024
        ),
    )(*args)


def mix_kernel(a, C, T, hp, att_ref, on_ref, ob_ref, stream_ref, gain_ref, gate_hbm, up_hbm, down_hbm,
               out_ref, gate_ref, up_ref, down_ref, pbuf, prec, mid, xs, pb, pr, rsum, ps,
               w_s, p_s, p_r, x_s, x_r, f_s, f_r, g_s, g_r, r_s, r_r):
    me = lax.axis_index("sp")
    j = lax.axis_index("tp")
    z, c = me // C, me % C
    share = out_ref.shape[0]
    fetch = [
        pltpu.make_async_copy(src, dst, w_s.at[i])
        for i, (src, dst) in enumerate(((gate_hbm, gate_ref), (up_hbm, up_ref), (down_hbm, down_ref)))
    ]
    for copy in fetch:
        copy.start()

    def along(k):
        return lax.rem(z + jnp.where(z < a // 2, k, a - k), a)

    def core(t):
        return lax.rem(j + t, T)

    greet([(lambda t: {"sp": lax.rem(z + t, a) * C + c}, a), (lambda t: {"tp": core(t)}, T)])

    cut = [att_ref[h][:, :NARROW_SIZE] for h in range(hp)]
    part = jnp.dot(jnp.concatenate(cut, axis=1), on_ref[...], preferred_element_type=jnp.float32)
    part = part + jnp.dot(
        jnp.concatenate([att_ref[hp + h] for h in range(hp)], axis=1), ob_ref[...],
        preferred_element_type=jnp.float32,
    )
    pbuf[...] = part.astype(jnp.bfloat16).reshape(pbuf.shape)

    def p_copy(to, src, t):
        return pltpu.make_async_remote_copy(
            src_ref=pbuf.at[to], dst_ref=prec.at[src], send_sem=p_s.at[t], recv_sem=p_r.at[src],
            device_id={"tp": to}, device_id_type=MESH)

    for t in range(1, T):
        p_copy(core(t), j, t).start()
    total = pbuf[j].astype(jnp.float32)
    for t in range(1, T):
        src = core(t)
        p_copy(src, src, t).wait_recv()
        total = total + prec[src].astype(jnp.float32)
    own = pl.ds(pl.multiple_of(j * share, share), share)
    mid[...] = (stream_ref[own, :].astype(jnp.float32) + total).astype(jnp.bfloat16)
    middle = mid[...].astype(jnp.float32)
    scaled = middle * lax.rsqrt(jnp.mean(middle * middle, axis=1, keepdims=True) + norm_eps)
    xs[z, j] = (scaled * gain_ref[...]).astype(jnp.bfloat16)

    def x_copy(m, src, k):
        return pltpu.make_async_remote_copy(
            src_ref=xs.at[src, j], dst_ref=xs.at[src, j], send_sem=x_s.at[k], recv_sem=x_r.at[src],
            device_id={"sp": m * C + c}, device_id_type=MESH)

    def f_copy(m, to, src, t):
        return pltpu.make_async_remote_copy(
            src_ref=xs.at[m, src], dst_ref=xs.at[m, src], send_sem=f_s.at[m, t], recv_sem=f_r.at[m, src],
            device_id={"tp": to}, device_id_type=MESH)

    def g_copy(m, to, src, t):
        return pltpu.make_async_remote_copy(
            src_ref=pb.at[m, to], dst_ref=pr.at[m, src], send_sem=g_s.at[m, t], recv_sem=g_r.at[m, src],
            device_id={"tp": to}, device_id_type=MESH)

    def r_copy(m, src):
        return pltpu.make_async_remote_copy(
            src_ref=rsum.at[m], dst_ref=ps.at[src], send_sem=r_s.at[m], recv_sem=r_r.at[src],
            device_id={"sp": m * C + c}, device_id_type=MESH)

    for k in range(1, a):
        x_copy(along(k), z, k).start()

    def join(m):
        total = pb[m, j].astype(jnp.float32)
        for t in range(1, T):
            g_copy(m, core(t), core(t), t).wait_recv()
            total = total + pr[m, core(t)].astype(jnp.float32)
        rsum[m] = total.astype(jnp.bfloat16)

    def one_member(k, carry):
        m = along(k)

        @pl.when(k > 0)
        def _():
            x_copy(m, m, 0).wait_recv()

        for t in range(1, T):
            f_copy(m, core(t), j, t).start()

        @pl.when(k == 0)
        def _():
            for copy in fetch:
                copy.wait()

        @pl.when(k > 1)
        def _():
            join(along(k - 1))
            r_copy(along(k - 1), z).start()

        for t in range(1, T):
            f_copy(m, core(t), core(t), t).wait_recv()
        x = xs[m].reshape(T * share, xs.shape[3])
        gate = jnp.dot(x, gate_ref[...], preferred_element_type=jnp.float32)
        up = jnp.dot(x, up_ref[...], preferred_element_type=jnp.float32)
        hidden = (gate / (1.0 + jnp.exp(-gate)) * up).astype(jnp.bfloat16)
        mixed = jnp.dot(hidden, down_ref[...], preferred_element_type=jnp.float32)
        pb[m] = mixed.astype(jnp.bfloat16).reshape(T, share, mixed.shape[1])
        for t in range(1, T):
            g_copy(m, core(t), j, t).start()
        return carry

    lax.fori_loop(0, a, one_member, 0)
    if a > 1:
        join(along(a - 1))
        r_copy(along(a - 1), z).start()
    join(z)
    total = rsum[z].astype(jnp.float32)
    for k in range(1, a):
        m = along(k)
        r_copy(m, m).wait_recv()
        total = total + ps[m].astype(jnp.float32)
    out_ref[...] = (mid[...].astype(jnp.float32) + total).astype(jnp.bfloat16)
    for t in range(1, T):
        p_copy(core(t), j, t).wait_send()
        for m in range(a):
            f_copy(m, core(t), j, t).wait_send()
            g_copy(m, core(t), j, t).wait_send()
    for k in range(1, a):
        x_copy(along(k), z, k).wait_send()
        r_copy(along(k), z).wait_send()


def mix(n, a, T, hp, att, out_narrow, out_broad, stream, gain, gate, up, down):
    rows, width = stream.shape
    share = rows // T
    dma = pltpu.SemaphoreType.DMA
    block = pltpu.VMEM((a, T, share, width), jnp.bfloat16)
    line = pltpu.VMEM((a, share, width), jnp.bfloat16)
    pair = pltpu.VMEM((T, share, width), jnp.bfloat16)
    vmem = pl.BlockSpec(memory_space=pltpu.VMEM)
    hbm = pl.BlockSpec(memory_space=pl.ANY)
    return pl.pallas_call(
        functools.partial(mix_kernel, a, n // a, T, hp),
        out_shape=jax.ShapeDtypeStruct((share, width), jnp.bfloat16),
        in_specs=[vmem] * 5 + [hbm] * 3,
        out_specs=vmem,
        scratch_shapes=[
            pltpu.VMEM(gate.shape, gate.dtype), pltpu.VMEM(up.shape, up.dtype),
            pltpu.VMEM(down.shape, down.dtype),
            pair, pair, pltpu.VMEM((share, width), jnp.bfloat16), block, block, block, line, line,
            dma((3,)), dma((T,)), dma((T,)), dma((a,)), dma((a,)), dma((a, T)), dma((a, T)),
            dma((a, T)), dma((a, T)), dma((a,)), dma((a,)),
        ],
        compiler_params=pltpu.CompilerParams(
            collective_id=1, has_side_effects=True, vmem_limit_bytes=60 * 1024 * 1024
        ),
    )(att, out_narrow, out_broad, stream, gain.reshape(1, width), gate, up, down)


def split_heads(array, heads, size):
    cut = jnp.transpose(array.reshape(array.shape[0], heads, size), (1, 0, 2))
    return jnp.pad(cut, ((0, 0), (0, 0), (0, WIDE - size)))


def local(n, T,
    stream,
    query_narrow,
    query_broad,
    key_narrow,
    key_broad,
    value_narrow,
    value_broad,
    key_offsets,
    out_narrow,
    out_broad,
    norm_gain,
    gate_weight,
    up_weight,
    down_weight,
):
    rows = stream.shape[0]
    hp = query_narrow.shape[1] // NARROW_SIZE

    def both(narrow, broad):
        return jnp.concatenate(
            [split_heads(narrow, hp, NARROW_SIZE), split_heads(broad, hp, BROAD_SIZE)], axis=0
        )

    q = both(query_narrow, query_broad)
    kv = jnp.stack([both(key_narrow, key_broad), both(value_narrow, value_broad)], axis=1)
    off = jnp.transpose(jnp.concatenate([key_offsets[:, 0::2], key_offsets[:, 1::2]], axis=1))
    off = jnp.broadcast_to(off[:, None, :], (2 * hp, 8, rows))
    group = 0
    if gate_weight.shape[0] % 128 == 0 and down_weight.shape[1] % 128 == 0:
        for a in (1, 2, 4):
            if n % a == 0 and gate_weight.shape[1] % (128 * a) == 0:
                group = a
    if group:
        att, gate_all, up_all, down_all = attend(
            n, hp, rows, group, q, kv, off, (gate_weight, up_weight, down_weight)
        )
        return mix(
            n, group, T, hp, att, out_narrow, out_broad, stream, norm_gain, gate_all, up_all, down_all
        )
    att = attend(n, hp, rows, 0, q, kv, off, None)[0]
    attended_narrow = jnp.transpose(att[:hp, :, :NARROW_SIZE], (1, 0, 2)).reshape(rows, -1)
    attended_broad = jnp.transpose(att[hp:], (1, 0, 2)).reshape(rows, -1)
    share = rows // T
    own = lax.axis_index("tp") * share
    summed = lax.psum_scatter(
        (
            jnp.dot(attended_narrow, out_narrow, preferred_element_type=jnp.float32)
            + jnp.dot(attended_broad, out_broad, preferred_element_type=jnp.float32)
        ).astype(jnp.bfloat16),
        "tp",
        scatter_dimension=0,
        tiled=True,
    ).astype(jnp.float32)
    mid_own = (lax.dynamic_slice_in_dim(stream, own, share, 0).astype(jnp.float32) + summed).astype(
        jnp.bfloat16
    )
    middle = mid_own.astype(jnp.float32)
    scaled = middle * lax.rsqrt(jnp.mean(middle * middle, axis=1, keepdims=True) + norm_eps)
    normed = lax.all_gather((scaled * norm_gain).astype(jnp.bfloat16), "tp", axis=0, tiled=True)
    part_gate = lax.all_gather(gate_weight, "sp", axis=0, tiled=True)
    part_up = lax.all_gather(up_weight, "sp", axis=0, tiled=True)
    gate = jnp.dot(normed, part_gate, preferred_element_type=jnp.float32)
    up = jnp.dot(normed, part_up, preferred_element_type=jnp.float32)
    hidden = (jax.nn.silu(gate) * up).astype(jnp.bfloat16)
    down_full = lax.all_gather(down_weight, "sp", axis=1, tiled=True)
    mixed = lax.psum_scatter(
        jnp.dot(
            hidden,
            down_full,
            preferred_element_type=jnp.float32,
        ).astype(jnp.bfloat16),
        "tp",
        scatter_dimension=0,
        tiled=True,
    ).astype(jnp.float32)
    return (mid_own.astype(jnp.float32) + mixed).astype(jnp.bfloat16)


def solution(mesh):
    placed = (
        P("sp", None),
        P("sp", "tp"),
        P("sp", "tp"),
        P("sp", "tp"),
        P("sp", "tp"),
        P("sp", "tp"),
        P("sp", "tp"),
        P("sp", "tp"),
        P("tp", None),
        P("tp", None),
        P(),
        P("sp", "tp"),
        P("sp", "tp"),
        P("tp", "sp"),
    )
    body = functools.partial(local, mesh.shape["sp"], mesh.shape["tp"])
    return jax.shard_map(
        body, mesh=mesh, in_specs=placed, out_specs=P(("sp", "tp"), None), check_vma=False
    )
```
